128 devices in a mesh: sp: 16 (over z, x), tp: 8 (over y, core).
Axes of the slice: x: 4, y: 4, z: 4, core: 2. Of those that a mesh axis runs over, the one named last changes fastest.
Arguments:
- queries: bfloat16 [16384, 512], P('sp', 'tp'), may hold values from -9.5625 to 9.5625
- keys: bfloat16 [16384, 512], P('sp', 'tp'), may hold values from -9.5625 to 9.5625
- values: bfloat16 [16384, 512], P('sp', 'tp'), may hold values from -6 to 6
- key_bias: bfloat16 [16384, 8], P('sp', 'tp'), may hold values from -17 to 0
- residual: bfloat16 [16384, 2048], P(('sp', 'tp')), may hold values from -6 to 6
- out_weight: bfloat16 [512, 2048], replicated, may hold values from -1 to 1
- norm_gain: float32 [2048], replicated, may hold values from 0.1 to 1.9
- routes: int32 [16384, 2], P(('sp', 'tp')), may hold values from 0 to 15, all different within a row; in each aligned block of 128 rows (0 to 127, 128 to 255, ...) at most 20 rows name the same one
- route_weights: float32 [16384, 2], P(('sp', 'tp')), may hold values from 0.25 to 2
- gate_weight: bfloat16 [16, 2048, 4096], P('sp', None, 'tp'), may hold values from -0.125 to 0.125
- up_weight: bfloat16 [16, 2048, 4096], P('sp', None, 'tp'), may hold values from -0.125 to 0.125
- down_weight: bfloat16 [16, 4096, 2048], P('sp', 'tp'), may hold values from -0.09375 to 0.09375
Outputs:
- output: bfloat16 [16384, 2048], P(('sp', 'tp'))
The draws below stay inside these ranges and needn't reach their ends.
Inputs may be any that keep to these rules, and one draw needn't show every extreme that they name: `routes`: each row names 2 different experts; the rows of one device name no expert more than 20 times.
All inputs are finite; a program needn't handle non-finite values.
Results may differ from the reference program's by a relative error of at most 0.017.
Values may be sent and summed in bfloat16 or wider, within the bound.
A program may use at most 128 MiB of HBM per device.

```python
import math
import jax
import jax.numpy as jnp
import numpy as np
from jax import lax

D = 2048
HEAD_COUNT = 8
HEAD_DIM = 64
FF = 4096
TOP = 2
SPAN = 512
TOK_DEV = 128
TOK_SP = 1024
SEQUENCE_LENGTH = 16384
EXPERTS = 16
CAP = 20
N_SP = 16
N_TP = 8


def draw_key_bias(key, part):
    gathered_keys = jax.random.split(jax.random.fold_in(key, 7), 6)
    fast_share = 0.5
    is_fast = jax.random.uniform(gathered_keys[0], (HEAD_COUNT,), jnp.float32) < fast_share
    slow_level = -jnp.log(jnp.float32(SEQUENCE_LENGTH)) - 3.0 + jax.random.uniform(gathered_keys[1], (HEAD_COUNT,), jnp.float32, minval=-0.5, maxval=0.5)
    fast_level = jax.random.uniform(gathered_keys[2], (HEAD_COUNT,), jnp.float32, minval=-7.0, maxval=-5.5)
    level = jnp.where(is_fast, fast_level, slow_level)
    block_shift = jnp.repeat(jax.random.uniform(gathered_keys[3], (N_SP,), jnp.float32, minval=-0.7, maxval=0.7), TOK_SP, total_repeat_length=SEQUENCE_LENGTH)
    sudden_position = jax.random.randint(gathered_keys[4], (4,), 0, SEQUENCE_LENGTH)
    sudden_value = jax.random.uniform(gathered_keys[5], (4, HEAD_COUNT), jnp.float32, minval=-1.5, maxval=0.0)
    position_index = jnp.arange(SEQUENCE_LENGTH, dtype=jnp.int32)
    sudden_hit_mask = (position_index[:, None] == sudden_position[None, :]).astype(jnp.float32)
    any_hit_flag = jnp.sum(sudden_hit_mask, axis=1, keepdims=True) > 0.0
    sudden_rows = jnp.dot(sudden_hit_mask, sudden_value)
    regular_rows = level[None, :] + block_shift[:, None]
    return jnp.where(any_hit_flag, sudden_rows, regular_rows).astype(jnp.bfloat16)


def levels(key, extent, pieces, smallest, high):
    factor_of = 1.0
    for position, shards_of in pieces:
        steps = jax.random.uniform(jax.random.fold_in(jax.random.fold_in(key, 6), position), (shards_of,), jnp.float32, smallest / len(pieces), high / len(pieces))
        factor_of = factor_of * jnp.repeat(jnp.exp(steps), extent[position] // shards_of).reshape((-1,) + (1,) * (len(extent) - 1 - position))
    return factor_of


def shared_out(own_key, own, number, rows, number_of, top, most, lean):
    ranking = jax.random.permutation(own_key, number_of)
    crowded, ordinary = load_shares(number_of, rows * top, most, lean, True), load_shares(number_of, rows * top, most, lean, False)
    places = jnp.arange(number_of)

    def named(lengths, offset_by):
        used = int((lengths > 0).sum())
        fixed = max(1, used // 4)
        shifted = fixed + (places - fixed + offset_by * (used - fixed)) % max(1, number_of - fixed)
        return jnp.zeros((number_of,), jnp.int32).at[ranking[jnp.where(places < fixed, places, shifted)]].set(jnp.asarray(lengths, jnp.int32))

    lengths = jnp.where(number % 4 == 0, named(crowded, number // 4), named(ordinary, number - number // 4 - 1))
    mixed = jax.random.permutation(jax.random.fold_in(own, 3), number_of)
    source_of, taker = mixed[0:number_of // 2 * 2:2], mixed[1:number_of // 2 * 2:2]
    room = jnp.minimum(lengths[source_of] - 1, most - lengths[taker]) // 2
    room = jnp.where((source_of == ranking[0]) | (taker == ranking[0]) | (lengths[taker] == 0), 0, jnp.maximum(room, 0))
    shifted = jax.random.randint(jax.random.fold_in(own, 4), (number_of // 2,), 0, 1 << 20) % (room + 1)
    lengths = lengths.at[source_of].add(-shifted).at[taker].add(shifted)
    labels = jnp.searchsorted(jnp.cumsum(lengths), jnp.arange(rows * top), side="right").astype(jnp.int32)
    table = labels.reshape(top, rows).T
    table = table[jax.random.permutation(jax.random.fold_in(own, 1), rows)]
    offset_by = jax.random.randint(jax.random.fold_in(own, 2), (rows, 1), 0, top)
    return jnp.take_along_axis(table, (jnp.arange(top)[None, :] + offset_by) % top, axis=1)


def load_shares(amount, total, reach, slope, full):
    portions = [(1 << 20) // math.isqrt(rank ** slope) + 1 for rank in range(1, amount + 1)]
    largest = reach if full else min(reach, max(-(-total // amount), total * portions[0] // sum(portions)))
    least = 1 if total - largest >= amount - 1 else 0
    given, rest = [largest] + [least] * (amount - 1), total - largest - least * (amount - 1)
    while rest > 0:
        candidates = [i for i in range(1, amount) if given[i] < largest] or [i for i in range(1, amount) if given[i] < reach]
        whole, left = sum([portions[i] for i in candidates]), rest
        for i in candidates:
            more = min(reach - given[i], max(1, left * portions[i] // whole), rest)
            given[i] = given[i] + more
            rest = rest - more
    return np.array(given)


def normal_values(rng, shape, width, bound, pieces=(), held_as=jnp.bfloat16):
    result = jax.random.normal(rng, shape, jnp.float32) * width
    if len(pieces) > 0:
        result = levels(rng, shape, pieces, -0.22, 0.18) * result
    return jnp.clip(result, min=-bound, max=bound).astype(held_as)


def setup_inputs(seed: int = 0) -> dict:
    splits = jax.random.split(jax.random.key(seed), 13)
    queries = normal_values(splits[0], (SEQUENCE_LENGTH, HEAD_COUNT * HEAD_DIM), 1.6, 9.5625, ((0, 16), (1, 8)))
    keys = normal_values(splits[1], (SEQUENCE_LENGTH, HEAD_COUNT * HEAD_DIM), 1.6, 9.5625, ((0, 16), (1, 8)))
    values = normal_values(splits[2], (SEQUENCE_LENGTH, HEAD_COUNT * HEAD_DIM), 1.0, 6.0, ((0, 16), (1, 8)))
    key_bias = draw_key_bias(jax.random.fold_in(splits[12], 71), 0)
    residual = normal_values(splits[4], (SEQUENCE_LENGTH, D), 1.0, 6.0, ((0, 128),))
    out_weight = normal_values(splits[5], (HEAD_COUNT * HEAD_DIM, D), (HEAD_COUNT * HEAD_DIM // 16) ** -0.5, 1.0)
    norm_gain = jnp.clip(1.0 + 0.18 * jax.random.normal(splits[6], (D,), jnp.float32), 0.1, 1.9)
    routes_keys = jax.random.split(jax.random.fold_in(splits[7], 1), SEQUENCE_LENGTH // TOK_DEV)
    routes_turns = jax.random.permutation(jax.random.fold_in(splits[7], 3), SEQUENCE_LENGTH // TOK_DEV)
    routes = jax.vmap(lambda own, number: shared_out(jax.random.fold_in(splits[7], 2), own, number, TOK_DEV, EXPERTS, TOP, CAP, 1))(routes_keys, routes_turns).reshape((SEQUENCE_LENGTH, TOP))
    route_weights = jnp.clip(jnp.exp(math.log(2.0) - 2.0794415 * jax.random.uniform(splits[8], (SEQUENCE_LENGTH, TOP), jnp.float32) ** levels(splits[8], (SEQUENCE_LENGTH, TOP), ((0, 128),), -0.2, 0.2)), 0.25, 2.0)
    gate_weight = normal_values(splits[9], (EXPERTS, D, FF), D ** -0.5, 0.125, ((0, 16), (2, 8)))
    up_weight = normal_values(splits[10], (EXPERTS, D, FF), D ** -0.5, 0.125, ((0, 16), (2, 8)))
    down_weight = normal_values(splits[11], (EXPERTS, FF, D), FF ** -0.5, 0.09375, ((0, 16), (1, 8)))
    return {"queries": queries, "keys": keys, "values": values, "key_bias": key_bias, "residual": residual, "out_weight": out_weight, "norm_gain": norm_gain, "routes": routes, "route_weights": route_weights, "gate_weight": gate_weight, "up_weight": up_weight, "down_weight": down_weight}


epsilon = 1e-06

def stick_span(query_block, key_block, value_block, bias_block, query_pos, key_pos):
    scores = jnp.einsum('qhd,khd->qhk', query_block, key_block) * HEAD_DIM ** (-0.5)
    scores = scores + jnp.transpose(bias_block)[None, :, :]
    earlier = key_pos[None, None, :] < query_pos[:, None, None]
    failure = jnp.where(earlier, jax.nn.log_sigmoid(-scores), 0.0)
    later_sum = lax.cumsum(failure, axis=2, reverse=True) - failure
    weights = jnp.where(earlier, jnp.exp(jax.nn.log_sigmoid(scores) + later_sum), 0.0).astype(jnp.bfloat16)
    span_out = jnp.einsum('qhk,khd->qhd', weights.astype(jnp.float32), value_block)
    return (span_out, lax.optimization_barrier(jnp.sum(failure, axis=2)))

def attend(queries, keys, values, key_bias):
    span_count = SEQUENCE_LENGTH // SPAN
    query_spans = queries.astype(jnp.float32).reshape(span_count, SPAN, HEAD_COUNT, HEAD_DIM)
    key_spans = keys.astype(jnp.float32).reshape(span_count, SPAN, HEAD_COUNT, HEAD_DIM)
    value_spans = values.astype(jnp.float32).reshape(span_count, SPAN, HEAD_COUNT, HEAD_DIM)
    bias_spans = key_bias.astype(jnp.float32).reshape(span_count, SPAN, HEAD_COUNT)

    def per_block(inputs):
        query_block, block_index = inputs
        query_pos = block_index * SPAN + jnp.arange(SPAN, dtype=jnp.int32)

        def step(held, key_index):
            running, after_total = held

            def compute():
                key_pos = key_index * SPAN + jnp.arange(SPAN, dtype=jnp.int32)
                return stick_span(query_block, key_spans[key_index], value_spans[key_index], bias_spans[key_index], query_pos, key_pos)

            def skipped():
                return (jnp.zeros((SPAN, HEAD_COUNT, HEAD_DIM), jnp.float32), jnp.zeros((SPAN, HEAD_COUNT), jnp.float32))
            span_out, span_sum = lax.cond(key_index <= block_index, compute, skipped)
            return ((running + jnp.exp(after_total)[..., None] * span_out, after_total + span_sum), None)
        start_pair = (jnp.zeros((SPAN, HEAD_COUNT, HEAD_DIM), jnp.float32), jnp.zeros((SPAN, HEAD_COUNT), jnp.float32))
        (running, _), _ = lax.scan(step, start_pair, jnp.arange(span_count, dtype=jnp.int32), reverse=True)
        return running.astype(jnp.bfloat16)
    blocks = lax.map(per_block, (query_spans, jnp.arange(span_count, dtype=jnp.int32)))
    return blocks.reshape(SEQUENCE_LENGTH, HEAD_COUNT * HEAD_DIM)

def experts_out(normed, routes, route_weights, gate_weight, up_weight, down_weight):
    most_rows = SEQUENCE_LENGTH // TOK_DEV * CAP
    flat_routes = routes.reshape(-1)
    flat_weights = route_weights.reshape(-1)
    token_of = (jnp.arange(SEQUENCE_LENGTH * TOP, dtype=jnp.int32) // TOP).astype(jnp.int32)
    block_units = FF // N_TP

    def one_expert(total, expert_index):
        chosen = flat_routes == expert_index
        picked = jnp.nonzero(chosen, size=most_rows, fill_value=0)[0].astype(jnp.int32)
        row_valid = jnp.arange(most_rows, dtype=jnp.int32) < jnp.sum(chosen.astype(jnp.int32))
        token_ids = token_of[picked]
        row_block = normed[token_ids]
        gate_act = jnp.dot(row_block, gate_weight[expert_index], preferred_element_type=jnp.float32)
        up_act = jnp.dot(row_block, up_weight[expert_index], preferred_element_type=jnp.float32)
        hidden = (jax.nn.silu(gate_act) * up_act).astype(jnp.bfloat16)
        summed = jnp.zeros((most_rows, D), jnp.float32)
        for block in range(N_TP):
            lower = block * block_units
            partial_value = jnp.dot(hidden[:, lower:lower + block_units], down_weight[expert_index, lower:lower + block_units], preferred_element_type=jnp.float32)
            summed = summed + lax.optimization_barrier(partial_value.astype(jnp.bfloat16)).astype(jnp.float32)
        expert_rows = lax.optimization_barrier(summed.astype(jnp.bfloat16)).astype(jnp.float32)
        scaled = jnp.where(row_valid[:, None], flat_weights[picked][:, None] * expert_rows, 0.0)
        return (total.at[token_ids].add(scaled), None)
    routed, _ = lax.scan(one_expert, jnp.zeros((SEQUENCE_LENGTH, D), jnp.float32), jnp.arange(EXPERTS, dtype=jnp.int32))
    return routed

def reference(queries, keys, values, key_bias, residual, out_weight, norm_gain, routes, route_weights, gate_weight, up_weight, down_weight):
    attended = attend(queries, keys, values, key_bias)
    mixed_rows = (residual.astype(jnp.float32) + jnp.dot(attended, out_weight, preferred_element_type=jnp.float32)).astype(jnp.bfloat16)
    stream = mixed_rows.astype(jnp.float32)
    normed = (stream * lax.rsqrt(lax.optimization_barrier(jnp.mean(stream * stream, axis=-1, keepdims=True)) + epsilon) * norm_gain).astype(jnp.bfloat16)
    routed = experts_out(normed, routes, route_weights, gate_weight, up_weight, down_weight)
    return (stream + routed).astype(jnp.bfloat16)
```

```python
import functools

import jax
import jax.numpy as jnp
from jax import lax
from jax.experimental import pallas as pl
from jax.experimental.pallas import tpu as pltpu
from jax.sharding import PartitionSpec as P

HEAD_DIM = 64
TOP = 2
LOG2E = 1.4426950408889634
KEY_CHUNK = 256
ROW_TILE = 512
CHUNKS_PER_STEP = 4


epsilon = 1e-06


def joined_along(blocks, dim):
    blocks = jnp.moveaxis(blocks, 0, dim)
    shape = blocks.shape
    return blocks.reshape(*shape[:dim], shape[dim] * shape[dim + 1], *shape[dim + 2 :])


def on_gathered_pieces(array, axis, dim, apply, out_dim):
    size, width = (lax.axis_size(axis), array.shape[dim])
    count = 2 if width % 2 == 0 else 1
    finished, length = ([], width // count)
    for k in range(count):
        section = lax.slice_in_dim(array, k * length, (k + 1) * length, axis=dim)
        starts = jnp.arange(size) * width + k * length
        finished.append(jax.vmap(apply)(lax.all_gather(section, axis), starts))
    return joined_along(jnp.concatenate(finished, axis=out_dim + 1), out_dim)


def stick_chunk(q, kv, bias2, suffix, later, earlier):
    scores = lax.dot_general(q, kv, (((1,), (1,)), ((), ())), preferred_element_type=jnp.float32)
    z = scores * (HEAD_DIM**-0.5 * LOG2E) + bias2
    softplus = jnp.maximum(jnp.log(1.0 + jnp.exp2(jnp.minimum(z, 126.0))) * LOG2E, z)
    if earlier is not None:
        softplus = jnp.where(earlier, softplus, 0.0)
    after = jnp.dot(softplus.astype(jnp.bfloat16), suffix, preferred_element_type=jnp.float32)
    weights = jnp.exp2(z - softplus - after - jnp.concatenate([later, later], axis=1))
    if earlier is not None:
        weights = jnp.where(earlier, weights, 0.0)
    out = jnp.dot(weights.astype(jnp.bfloat16), kv, preferred_element_type=jnp.float32)
    return out, jnp.sum(softplus, axis=1, keepdims=True)


def attention_kernel(q_ref, kv_ref, bias_ref, suffix_ref, out_ref, total, later):
    me = lax.axis_index("sp")
    rows = q_ref.shape[0]
    own = rows // KEY_CHUNK
    total[...] = jnp.zeros_like(total)
    later[...] = jnp.zeros_like(later)

    def run(c, diagonal):
        kv = kv_ref[pl.ds(pl.multiple_of(c * KEY_CHUNK, KEY_CHUNK), KEY_CHUNK), :]
        bias2 = bias_ref[c]
        for first in range(0, rows, ROW_TILE):
            tile = pl.ds(first, ROW_TILE)
            earlier = None
            if diagonal:
                q_pos = me * rows + first + lax.broadcasted_iota(jnp.int32, (ROW_TILE, KEY_CHUNK), 0)
                k_pos = c * KEY_CHUNK + lax.broadcasted_iota(jnp.int32, (ROW_TILE, KEY_CHUNK), 1)
                earlier = k_pos < q_pos
            out, sums = stick_chunk(q_ref[tile, :], kv, bias2, suffix_ref[...], later[tile, :], earlier)
            total[tile, :] += out
            later[tile, :] += jnp.broadcast_to(sums, (ROW_TILE, 128))

    @pl.loop(0, own)
    def _(j):
        run(me * own + own - 1 - j, True)

    @pl.loop(0, me * own // CHUNKS_PER_STEP)
    def _(j):
        for u in range(CHUNKS_PER_STEP):
            run(me * own - 1 - j * CHUNKS_PER_STEP - u, False)

    out_ref[...] = total[...].astype(out_ref.dtype)


def attention(q, kv, bias2, suffix):
    rows = q.shape[0]
    return pl.pallas_call(
        attention_kernel,
        out_shape=jax.ShapeDtypeStruct((rows, 128), jnp.bfloat16),
        in_specs=[pl.BlockSpec(memory_space=pltpu.VMEM)] * 4,
        out_specs=pl.BlockSpec(memory_space=pltpu.VMEM),
        scratch_shapes=[pltpu.VMEM((rows, 128), jnp.float32), pltpu.VMEM((rows, 128), jnp.float32)],
        compiler_params=pltpu.CompilerParams(vmem_limit_bytes=40 << 20),
        cost_estimate=pl.CostEstimate(flops=20_000_000_000, bytes_accessed=5_000_000, transcendentals=0),
        name="attention",
    )(q, kv, bias2, suffix)


def shards(
    queries,
    keys,
    values,
    key_bias,
    residual,
    out_weight,
    norm_gain,
    routes,
    route_weights,
    gate_weight,
    up_weight,
    down_weight,
):
    sp_count = lax.axis_size("sp")
    kv = lax.all_gather(jnp.concatenate([keys, values], axis=1), "sp", axis=0, tiled=True)
    bias = lax.all_gather(key_bias.reshape(1, -1), "sp", axis=0, tiled=True)
    bias2 = (bias.astype(jnp.float32) * LOG2E).reshape(-1, 1, KEY_CHUNK)
    order = lax.iota(jnp.int32, KEY_CHUNK)
    suffix = (order[:, None] > order[None, :]).astype(jnp.bfloat16)
    attended = attention(jnp.pad(queries, ((0, 0), (0, 128 - HEAD_DIM))), kv, bias2, suffix)[:, HEAD_DIM:]
    token_heads = lax.all_to_all(attended, "tp", split_axis=0, concat_axis=1, tiled=True)
    projected = jnp.dot(token_heads, out_weight, preferred_element_type=jnp.float32)
    stream = (residual.astype(jnp.float32) + projected).astype(jnp.bfloat16).astype(jnp.float32)
    normed = (
        stream * lax.rsqrt(jnp.mean(stream * stream, axis=-1, keepdims=True) + epsilon) * norm_gain
    ).astype(jnp.bfloat16)
    token_count = residual.shape[0]
    width_model = residual.shape[1]
    capacity = max(2, 5 * token_count * TOP // (4 * sp_count))
    flat_routes = routes.reshape(-1)
    onehot = (flat_routes[:, None] == lax.iota(jnp.int32, sp_count)[None, :]).astype(jnp.int32)
    before = jnp.cumsum(onehot, axis=0) - onehot
    slot_of = flat_routes * capacity + jnp.sum(before * onehot, axis=1)
    select = (slot_of[:, None] == lax.iota(jnp.int32, sp_count * capacity)[None, :]).astype(
        jnp.bfloat16
    )
    placing = jnp.sum(select.reshape(token_count, TOP, sp_count * capacity), axis=1)
    outgoing = jnp.einsum("ts,td->sd", placing, normed, preferred_element_type=jnp.float32).astype(
        jnp.bfloat16
    )
    arrived = lax.all_to_all(outgoing, "sp", split_axis=0, concat_axis=0, tiled=True)

    def fan_hidden(row_block, first_row):
        gate_act = jnp.dot(row_block, gate_weight[0], preferred_element_type=jnp.float32)
        up_act = jnp.dot(row_block, up_weight[0], preferred_element_type=jnp.float32)
        return (jax.nn.silu(gate_act) * up_act).astype(jnp.bfloat16)

    hidden = on_gathered_pieces(arrived, "tp", 0, fan_hidden, 0)
    partial_value = jnp.dot(hidden, down_weight[0], preferred_element_type=jnp.float32)
    summed = lax.psum_scatter(
        lax.optimization_barrier(partial_value.astype(jnp.bfloat16))
        .astype(jnp.float32)
        .astype(jnp.bfloat16),
        "tp",
        scatter_dimension=0,
        tiled=True,
    )
    returned = lax.all_to_all(summed, "sp", split_axis=0, concat_axis=0, tiled=True)
    picked = jnp.dot(select, returned, preferred_element_type=jnp.float32).reshape(
        token_count, TOP, width_model
    )
    routed = jnp.sum(picked * route_weights[:, :, None], axis=1)
    return (stream + routed).astype(jnp.bfloat16)


def solution(mesh):
    return jax.shard_map(
        shards,
        mesh=mesh,
        in_specs=(
            P("sp", "tp"),
            P("sp", "tp"),
            P("sp", "tp"),
            P("sp", "tp"),
            P(("sp", "tp"), None),
            P(),
            P(),
            P(("sp", "tp"), None),
            P(("sp", "tp"), None),
            P("sp", None, "tp"),
            P("sp", None, "tp"),
            P("sp", "tp", None),
        ),
        out_specs=P(("sp", "tp"), None),
        check_vma=False,
    )
```
